32 devices in a mesh: fs: 4 (over y, x), tp: 8 (over z, core).
Axes of the slice: x: 2, y: 2, z: 4, core: 2. Of those that a mesh axis runs over, the one named last changes fastest.
Arguments:
- tokens: bfloat16 [4096, 2048], P(('fs', 'tp')), may hold values from -6 to 6
- gate_weight: bfloat16 [2048, 5632], P('fs', 'tp'), may hold values from -0.125 to 0.125
- up_weight: bfloat16 [2048, 5632], P('fs', 'tp'), may hold values from -0.125 to 0.125
- down_weight: bfloat16 [5632, 2048], P('tp', 'fs'), may hold values from -0.078125 to 0.078125
- grad_out: bfloat16 [4096, 2048], P(('fs', 'tp')), may hold values from -6 to 6
Outputs:
- grad_input: bfloat16 [4096, 2048], P(('fs', 'tp'))
- grad_gate: float32 [2048, 5632], P('fs', 'tp')
- grad_up: float32 [2048, 5632], P('fs', 'tp')
- grad_down: float32 [5632, 2048], P('tp', 'fs')
The draws below stay inside these ranges and needn't reach their ends.
All inputs are finite; a program needn't handle non-finite values.
Results may differ from the reference program's by a relative error of at most 0.0049.
Values may be sent and summed in bfloat16 or wider, within the bound.
A program may use at most 128 MiB of HBM per device.

```python
import jax
import jax.numpy as jnp

D = 2048
FF = 5632
TOKENS = 4096


def spiked(array, key, source, target, parts, factor):
    owner, partner = [(jnp.arange(array.shape[dim]) // (array.shape[dim] // parts)).reshape([-1 if axis == dim else 1 for axis in range(array.ndim)]) for dim in (source, target)]
    chosen = jax.random.permutation(key, parts)[partner]
    strong = (owner == chosen) | (owner == (partner + parts // 2) % parts)
    return jnp.where(strong, factor * array, array)


def shard_levels(own_key, dims, shards, least, high):
    factor_of, own = 1.0, jax.random.fold_in(own_key, 6)
    for position, shards_of in shards:
        draws = jnp.exp(jax.random.uniform(jax.random.fold_in(own, position), (shards_of,), jnp.float32, least / len(shards), high / len(shards)))
        factor_of = factor_of * jnp.repeat(draws, dims[position] // shards_of).reshape([-1 if axis == position else 1 for axis in range(len(dims))])
    return factor_of


def bell_draw(own_key, dims, spread, limit, split=(), held_as=jnp.bfloat16):
    factor_of = shard_levels(own_key, dims, split, -0.22, 0.18) if split else 1.0
    result = jax.random.normal(own_key, dims, jnp.float32) * spread * factor_of
    return jnp.minimum(jnp.maximum(result, -limit), limit).astype(held_as)


def gaussian_with(key, extent, width, bound, shards, heavy, held_as=jnp.bfloat16):
    entries = width * jax.random.normal(key, extent, jnp.float32)
    if shards:
        entries = entries * shard_levels(key, extent, shards, -0.22, 0.18)
    return jnp.clip(spiked(entries, jax.random.fold_in(key, 3), *heavy), -bound, bound).astype(held_as)


def setup_inputs(seed: int = 0) -> dict:
    splits = jax.random.split(jax.random.key(seed), 6)
    tokens = bell_draw(splits[0], (TOKENS, D), 1.0, 6.0, ((0, 32),))
    gate_weight = bell_draw(splits[1], (D, FF), D ** -0.5, 0.125, ((0, 4), (1, 8)))
    up_weight = bell_draw(splits[2], (D, FF), D ** -0.5, 0.125, ((0, 4), (1, 8)))
    down_weight = bell_draw(splits[3], (FF, D), FF ** -0.5, 0.078125, ((0, 8), (1, 4)))
    grad_out = gaussian_with(splits[4], (TOKENS, D), 1.0, 6.0, ((0, 32),), (0, 1, 32, 2.75))
    return {"tokens": tokens, "gate_weight": gate_weight, "up_weight": up_weight, "down_weight": down_weight, "grad_out": grad_out}


def reference(tokens, gate_weight, up_weight, down_weight, grad_out):
    gate_pre = jnp.dot(tokens, gate_weight, preferred_element_type=jnp.float32)
    up_pre = jnp.dot(tokens, up_weight, preferred_element_type=jnp.float32)
    sig_gate = jax.nn.sigmoid(gate_pre)
    active = gate_pre * sig_gate
    hidden = (active * up_pre).astype(jnp.bfloat16)
    d_hidden = jnp.dot(grad_out, down_weight.T, preferred_element_type=jnp.float32)
    d_gate = (d_hidden * up_pre * sig_gate * (1.0 + gate_pre * (1.0 - sig_gate))).astype(jnp.bfloat16)
    d_up = (d_hidden * active).astype(jnp.bfloat16)
    grad_input = (jnp.dot(d_gate, gate_weight.T, preferred_element_type=jnp.float32)
                  + jnp.dot(d_up, up_weight.T, preferred_element_type=jnp.float32)).astype(jnp.bfloat16)
    grad_gate = jnp.dot(tokens.T, d_gate, preferred_element_type=jnp.float32)
    grad_up = jnp.dot(tokens.T, d_up, preferred_element_type=jnp.float32)
    grad_down = jnp.dot(hidden.T, grad_out, preferred_element_type=jnp.float32)
    return grad_input, grad_gate, grad_up, grad_down
```

```python
import functools

import jax
import jax.numpy as jnp
from jax import lax
from jax.experimental import pallas as pl
from jax.experimental.pallas import tpu as pltpu
from jax.sharding import PartitionSpec as P

MESH = pl.DeviceIdType.MESH
CORES = 2


def over_rows(left, right, out=jnp.float32):
    return lax.dot_general(
        left, right, (((0,), (0,)), ((), ())), preferred_element_type=jnp.float32
    ).astype(out)


def over_cols(left, right):
    return lax.dot_general(
        left, right, (((1,), (1,)), ((), ())), preferred_element_type=jnp.float32
    )


def orders_of(n_fs):
    bits = [1 << i for i in range(n_fs.bit_length() - 1)]
    return (bits, bits[::-1])


def first_bit(order, mask):
    return next(i for i, bit in enumerate(order) if mask & bit)


def greet(n_fs, depth, fs, tp, z):
    barrier = pltpu.get_barrier_semaphore()
    bits = orders_of(n_fs)[0]

    def hello(fs_id, tp_id):
        pl.semaphore_signal(barrier, inc=1, device_id=(fs_id, tp_id), device_id_type=MESH)

    for bit in bits:
        hello(fs ^ bit, tp)
    hello(fs, tp ^ 1)

    @pl.when(z > 0)
    def _():
        hello(fs, tp - CORES)

    @pl.when(z < depth - 1)
    def _():
        hello(fs, tp + CORES)

    ends = (z > 0).astype(jnp.int32) + (z < depth - 1).astype(jnp.int32)
    pl.semaphore_wait(barrier, len(bits) + 1 + ends)


def gather_kernel(n_fs, n_tp, *refs):
    ins, outs = refs[:5], refs[5:10]
    w_send, w_recv, z_send, z_recv, c_send, c_recv, l_sem = refs[10:]
    fs, tp = lax.axis_index("fs"), lax.axis_index("tp")
    depth = n_tp // CORES
    z = tp // CORES
    orders = orders_of(n_fs)
    phases = len(orders[0])
    weights = ((ins[1], outs[1], 0), (ins[2], outs[2], 0), (ins[3], outs[3], 1))
    rows = ((ins[0], outs[0]), (ins[4], outs[4]))
    greet(n_fs, depth, fs, tp, z)

    def w_block(array, split, owner):
        ref, out, axis = weights[array]
        half = ref.shape[0] // 2
        if axis == 0:
            own = ref.at[pl.ds(split * half, half), :]
            there = out.at[pl.ds(pl.multiple_of(owner * ref.shape[0] + split * half, half), half), :]
        else:
            own = ref.at[pl.ds(split * half, half), :]
            cols = ref.shape[1]
            there = out.at[pl.ds(split * half, half), pl.ds(pl.multiple_of(owner * cols, cols), cols)]
        return own, there

    def w_copy(array, split, phase, mask):
        own, there = w_block(array, split, fs ^ mask)
        order = orders[split]
        slot = (array, split, (1 << phase) - 1 + sum(1 << i for i in range(phase) if mask & order[i]))
        return pltpu.make_async_remote_copy(
            src_ref=own if mask == 0 else there,
            dst_ref=there,
            send_sem=w_send.at[slot],
            recv_sem=w_recv.at[slot],
            device_id=(fs ^ order[phase], tp),
            device_id_type=MESH,
        )

    def r_block(array, owner):
        ref, out = rows[array]
        n = ref.shape[0]
        return out.at[pl.ds(pl.multiple_of(owner * n, n), n), :]

    def z_copy(array, way, step):
        sign = 1 if way == 0 else -1
        there = r_block(array, tp - sign * step * CORES)
        return pltpu.make_async_remote_copy(
            src_ref=rows[array][0] if step == 0 else there,
            dst_ref=there,
            send_sem=z_send.at[array, way, step],
            recv_sem=z_recv.at[array, way, step],
            device_id=(fs, tp + sign * CORES),
            device_id_type=MESH,
        )

    def sends(way, step):
        if way == 0:
            return jnp.logical_and(z - step >= 0, z < depth - 1)
        return jnp.logical_and(z + step <= depth - 1, z > 0)

    def arrives(way, step):
        return z - 1 - step >= 0 if way == 0 else z + 1 + step <= depth - 1

    def c_copy(array, way, step):
        sign = 1 if way == 0 else -1
        there = r_block(array, tp - sign * (step + 1) * CORES)
        slot = (array, way, step + 1)
        return pltpu.make_async_remote_copy(
            src_ref=rows[array][0] if step == -1 else there,
            dst_ref=there,
            send_sem=c_send.at[slot],
            recv_sem=c_recv.at[slot],
            device_id=(fs, tp ^ 1),
            device_id_type=MESH,
        )

    for array in range(2):
        for way in range(2):

            @pl.when(sends(way, 0))
            def _():
                z_copy(array, way, 0).start()

    for phase in range(phases):
        for array in range(3):
            for split in range(2):
                w_copy(array, split, phase, 0).start()
    for array in range(2):
        c_copy(array, 0, -1).start()
    local = []
    for array in range(3):
        for split in range(2):
            own, there = w_block(array, split, fs)
            local.append((own, there))
    for array in range(2):
        local.append((rows[array][0], r_block(array, tp)))
    local = [pltpu.make_async_copy(a, b, l_sem.at[i]) for i, (a, b) in enumerate(local)]
    for copy in local:
        copy.start()

    def w_event(array, phase, index):
        for split in range(2):
            order = orders[split]
            mask = sum(order[i] for i in range(phase) if index & (1 << i))
            w_copy(array, split, phase, mask).wait_recv()
            got = mask | order[phase]
            for later in range(phase + 1, phases):
                w_copy(array, split, later, got).start()

    def z_event(array, way, step):
        @pl.when(arrives(way, step))
        def _():
            z_copy(array, way, step).wait_recv()
            c_copy(array, way, step).start()

        if step + 1 < depth - 1:

            @pl.when(sends(way, step + 1))
            def _():
                z_copy(array, way, step + 1).start()

    w_events = [
        functools.partial(w_event, array, phase, index)
        for phase in range(phases)
        for index in range(1 << phase)
        for array in range(3)
    ]
    z_events = [
        [functools.partial(z_event, array, way, step) for way in range(2)]
        for step in range(depth - 1)
        for array in range(2)
    ]
    for i in range(max(len(w_events), len(z_events))):
        if i < len(w_events):
            w_events[i]()
        if i < len(z_events):
            for event in z_events[i]:
                event()

    for copy in local:
        copy.wait()
    for array in range(2):
        c_copy(array, 0, -1).wait_send()
        c_copy(array, 0, -1).wait_recv()
        for way in range(2):
            for step in range(depth - 1):

                @pl.when(sends(way, step))
                def _():
                    z_copy(array, way, step).wait_send()

                @pl.when(arrives(way, step))
                def _():
                    c_copy(array, way, step).wait_send()
                    c_copy(array, way, step).wait_recv()

    for array in range(3):
        for split in range(2):
            order = orders[split]
            for phase in range(phases):
                for index in range(1 << phase):
                    mask = sum(order[i] for i in range(phase) if index & (1 << i))
                    w_copy(array, split, phase, mask).wait_send()


def gather_all(n_fs, n_tp, *ins):
    tokens, gate, up, down, cot = ins
    depth = n_tp // CORES
    any_spec = pl.BlockSpec(memory_space=pl.ANY)
    vmem = pl.BlockSpec(memory_space=pltpu.VMEM)
    full = lambda a, axis, n: jax.ShapeDtypeStruct(
        tuple(s * n if i == axis else s for i, s in enumerate(a.shape)), a.dtype
    )
    dma = pltpu.SemaphoreType.DMA
    return pl.pallas_call(
        functools.partial(gather_kernel, n_fs, n_tp),
        out_shape=(
            full(tokens, 0, n_tp),
            full(gate, 0, n_fs),
            full(up, 0, n_fs),
            full(down, 1, n_fs),
            full(cot, 0, n_tp),
        ),
        in_specs=[vmem] * 5,
        out_specs=[any_spec] * 5,
        scratch_shapes=[
            dma((3, 2, n_fs - 1)),
            dma((3, 2, n_fs - 1)),
            dma((2, 2, max(depth - 1, 1))),
            dma((2, 2, max(depth - 1, 1))),
            dma((2, 2, depth)),
            dma((2, 2, depth)),
            dma((8,)),
        ],
        compiler_params=pltpu.CompilerParams(collective_id=0, has_side_effects=True),
        name="gather",
    )(*ins)


def scatter_kernel(n_fs, n_tp, *refs):
    gi_ref, *w_refs = refs[:4]
    gi_out, *w_outs = refs[4:8]
    stages, recvs = refs[8:11], refs[11:14]
    c_buf, z_stage, z_buf = refs[14:17]
    w_send, w_recv, z_send, z_recv, c_send, c_recv = refs[17:]
    fs, tp = lax.axis_index("fs"), lax.axis_index("tp")
    depth = n_tp // CORES
    z, core = tp // CORES, tp % CORES
    orders = orders_of(n_fs)
    phases = len(orders[0])
    axes = (0, 0, 1)
    f32 = jnp.float32
    greet(n_fs, depth, fs, tp, z)

    def w_own(array, split, mask):
        out, axis = w_outs[array], axes[array]
        half = out.shape[0] // 2
        owner = fs ^ mask
        if axis == 0:
            start = pl.multiple_of(owner * out.shape[0] + split * half, half)
            return w_refs[array].at[pl.ds(start, half), :]
        cols = out.shape[1]
        return w_refs[array].at[
            pl.ds(split * half, half), pl.ds(pl.multiple_of(owner * cols, cols), cols)
        ]

    def compact(order, mask):
        return sum(1 << i for i, bit in enumerate(order) if mask & bit)

    def w_copy(array, split, mask):
        order = orders[split]
        phase = first_bit(order, mask)
        slot = compact(order, mask) - 1
        src = w_own(array, split, mask) if phase == 0 else stages[array].at[split, slot]
        return pltpu.make_async_remote_copy(
            src_ref=src,
            dst_ref=recvs[array].at[split, slot],
            send_sem=w_send.at[array, split, slot],
            recv_sem=w_recv.at[array, split, slot],
            device_id=(fs ^ order[phase], tp),
            device_id_type=MESH,
        )

    def w_sum(array, split, mask):
        order = orders[split]
        total = w_own(array, split, mask)[...].astype(f32)
        limit = phases if mask == 0 else first_bit(order, mask)
        for phase in range(limit):
            sent = mask | order[phase]
            w_copy(array, split, sent).wait_recv()
            total += recvs[array][split, compact(order, sent) - 1].astype(f32)
        return total

    n = gi_out.shape[0]

    def g_rows(target, which):
        return pl.ds(pl.multiple_of((target * CORES + which) * n, n), n)

    def c_copy(target):
        return pltpu.make_async_remote_copy(
            src_ref=gi_ref.at[g_rows(target, 1 - core), :],
            dst_ref=c_buf.at[target],
            send_sem=c_send.at[target],
            recv_sem=c_recv.at[target],
            device_id=(fs, tp ^ 1),
            device_id_type=MESH,
        )

    def z_target(way, step):
        return depth - 1 - step if way == 0 else step

    def z_copy(way, step):
        return pltpu.make_async_remote_copy(
            src_ref=z_stage.at[way, step],
            dst_ref=z_buf.at[way, step],
            send_sem=z_send.at[way, step],
            recv_sem=z_recv.at[way, step],
            device_id=(fs, tp + CORES if way == 0 else tp - CORES),
            device_id_type=MESH,
        )

    def sends(way, step):
        t = z_target(way, step)
        return t > z if way == 0 else t < z

    def arrives(way, step):
        t = z_target(way, step)
        return jnp.logical_and(z > 0, t >= z) if way == 0 else jnp.logical_and(z < depth - 1, t <= z)

    targets = []
    for i in range(depth):
        t = depth - 1 - i // 2 if i % 2 == 0 else i // 2
        targets.append(t)
    for t in targets:
        c_copy(t).start()

    for array in range(3):
        for split in range(2):
            order = orders[split]
            masks = [m for m in range(1, n_fs) if m & order[0]]
            for mask in sorted(masks, key=lambda m: -compact(order, m)):
                w_copy(array, split, mask).start()

    both = c_buf
    for t in targets:
        c_copy(t).wait_recv()
        both[t] = (
            both[t].astype(f32) + gi_ref[g_rows(t, core), :].astype(f32)
        ).astype(both.dtype)

    def z_event(way, step):
        t = z_target(way, step)

        @pl.when(arrives(way, step))
        def _():
            z_copy(way, step).wait_recv()

        @pl.when(sends(way, step))
        def _():
            @pl.when(arrives(way, step))
            def _():
                z_stage[way, step] = (
                    both[t].astype(f32) + z_buf[way, step].astype(f32)
                ).astype(z_stage.dtype)

            @pl.when(jnp.logical_not(arrives(way, step)))
            def _():
                z_stage[way, step] = both[t]

            z_copy(way, step).start()

    def w_event(array, mask):
        for split in range(2):
            order = orders[split]
            real = sum(bit for i, bit in enumerate(order) if mask & (1 << i))
            slot = mask - 1
            stages[array][split, slot] = w_sum(array, split, real).astype(stages[array].dtype)
            w_copy(array, split, real).start()

    def w_finish(array):
        half = w_outs[array].shape[0] // 2
        for split in range(2):
            w_outs[array][pl.ds(split * half, half), :] = w_sum(array, split, 0)

    later = [m for m in range(1, n_fs) if not m & 1]
    later = sorted(later, key=lambda m: ((m & -m), -m))
    w_events = [functools.partial(w_event, array, mask) for array in range(3) for mask in later]
    z_events = [
        functools.partial(z_event, way, step) for step in range(depth - 1) for way in range(2)
    ]
    per = -(-len(z_events) // max(len(w_events), 1))
    for i in range(max(len(w_events), -(-len(z_events) // per))):
        for event in z_events[i * per : (i + 1) * per]:
            event()
        if i < len(w_events):
            w_events[i]()

    total = both[z].astype(f32)
    zero = jnp.zeros_like(total)
    from_left = z_buf[0, jnp.clip(depth - 1 - z, 0, depth - 2)].astype(f32)
    from_right = z_buf[1, jnp.clip(z, 0, depth - 2)].astype(f32)
    total += jnp.where(z > 0, from_left, zero)
    total += jnp.where(z < depth - 1, from_right, zero)
    gi_out[...] = total.astype(gi_out.dtype)

    for array in range(3):
        w_finish(array)

    for t in targets:
        c_copy(t).wait_send()
    for way in range(2):
        for step in range(depth - 1):

            @pl.when(sends(way, step))
            def _():
                z_copy(way, step).wait_send()

    for array in range(3):
        for split in range(2):
            for mask in range(1, n_fs):
                w_copy(array, split, mask).wait_send()


def scatter_all(n_fs, n_tp, gi, gg, gu, gd):
    depth = n_tp // CORES
    f32 = jnp.float32
    vmem = pl.BlockSpec(memory_space=pltpu.VMEM)
    dma = pltpu.SemaphoreType.DMA
    shapes = (
        (gg.shape[0] // n_fs, gg.shape[1]),
        (gu.shape[0] // n_fs, gu.shape[1]),
        (gd.shape[0], gd.shape[1] // n_fs),
    )
    n, width = gi.shape[0] // n_tp, gi.shape[1]
    slots = [pltpu.VMEM((2, n_fs - 1, s[0] // 2, s[1]), gi.dtype) for s in shapes]
    return pl.pallas_call(
        functools.partial(scatter_kernel, n_fs, n_tp),
        out_shape=(jax.ShapeDtypeStruct((n, width), gi.dtype),)
        + tuple(jax.ShapeDtypeStruct(s, f32) for s in shapes),
        in_specs=[vmem] * 4,
        out_specs=[vmem] * 4,
        scratch_shapes=slots
        + slots
        + [
            pltpu.VMEM((depth, n, width), gi.dtype),
            pltpu.VMEM((2, depth - 1, n, width), gi.dtype),
            pltpu.VMEM((2, depth - 1, n, width), gi.dtype),
            dma((3, 2, n_fs - 1)),
            dma((3, 2, n_fs - 1)),
            dma((2, depth - 1)),
            dma((2, depth - 1)),
            dma((depth,)),
            dma((depth,)),
        ],
        compiler_params=pltpu.CompilerParams(
            collective_id=1, has_side_effects=True, vmem_limit_bytes=60 * 1024 * 1024
        ),
        name="scatter",
    )(gi, gg, gu, gd)


def body(n_fs, n_tp, tokens, gate_weight, up_weight, down_weight, grad_out):
    bf16 = tokens.dtype
    tok_all, gate_full, up_full, down_full, cot_all = gather_all(
        n_fs, n_tp, tokens, gate_weight, up_weight, down_weight, grad_out
    )
    gate_pre = jnp.dot(tok_all, gate_full, preferred_element_type=jnp.float32)
    up_pre = jnp.dot(tok_all, up_full, preferred_element_type=jnp.float32)
    sig_gate = jax.nn.sigmoid(gate_pre)
    active = gate_pre * sig_gate
    hidden = (active * up_pre).astype(bf16)
    d_hidden = over_cols(cot_all, down_full)
    d_gate = (d_hidden * up_pre * sig_gate * (1.0 + gate_pre * (1.0 - sig_gate))).astype(bf16)
    d_up = (d_hidden * active).astype(bf16)
    grad_input = (over_cols(d_gate, gate_full) + over_cols(d_up, up_full)).astype(bf16)
    return scatter_all(
        n_fs,
        n_tp,
        grad_input,
        over_rows(tok_all, d_gate, bf16),
        over_rows(tok_all, d_up, bf16),
        over_rows(hidden, cot_all, bf16),
    )


def solution(mesh):
    in_specs = (
        P(("fs", "tp"), None),
        P("fs", "tp"),
        P("fs", "tp"),
        P("tp", "fs"),
        P(("fs", "tp"), None),
    )
    out_specs = (P(("fs", "tp"), None), P("fs", "tp"), P("fs", "tp"), P("tp", "fs"))
    return jax.shard_map(
        functools.partial(body, mesh.shape["fs"], mesh.shape["tp"]),
        mesh=mesh,
        in_specs=in_specs,
        out_specs=out_specs,
        check_vma=False,
    )
```

```python
import functools

import jax
import jax.numpy as jnp
from jax import lax
from jax.experimental import pallas as pl
from jax.experimental.pallas import tpu as pltpu
from jax.sharding import PartitionSpec as P

MESH = pl.DeviceIdType.MESH
CORES = 2


def over_rows(left, right, out=jnp.float32):
    return lax.dot_general(
        left, right, (((0,), (0,)), ((), ())), preferred_element_type=jnp.float32
    ).astype(out)


def over_cols(left, right):
    return lax.dot_general(
        left, right, (((1,), (1,)), ((), ())), preferred_element_type=jnp.float32
    )


def orders_of(n_fs):
    bits = [1 << i for i in range(n_fs.bit_length() - 1)]
    return (bits, bits[::-1])


def first_bit(order, mask):
    return next(i for i, bit in enumerate(order) if mask & bit)


def greet(n_fs, depth, fs, tp, z):
    barrier = pltpu.get_barrier_semaphore()
    bits = orders_of(n_fs)[0]

    def hello(fs_id, tp_id):
        pl.semaphore_signal(barrier, inc=1, device_id=(fs_id, tp_id), device_id_type=MESH)

    for bit in bits:
        hello(fs ^ bit, tp)
    hello(fs, tp ^ 1)

    @pl.when(z > 0)
    def _():
        hello(fs, tp - CORES)

    @pl.when(z < depth - 1)
    def _():
        hello(fs, tp + CORES)

    ends = (z > 0).astype(jnp.int32) + (z < depth - 1).astype(jnp.int32)
    pl.semaphore_wait(barrier, len(bits) + 1 + ends)


def gather_kernel(n_fs, n_tp, *refs):
    ins, outs = refs[:5], refs[5:10]
    w_send, w_recv, z_send, z_recv, c_send, c_recv, l_sem = refs[10:]
    fs, tp = lax.axis_index("fs"), lax.axis_index("tp")
    depth = n_tp // CORES
    z = tp // CORES
    orders = orders_of(n_fs)
    phases = len(orders[0])
    weights = tuple((ins[i], outs[i]) for i in (1, 2, 3))
    rows = ((ins[0], outs[0]), (ins[4], outs[4]))
    greet(n_fs, depth, fs, tp, z)

    def w_block(array, split, owner):
        ref, out = weights[array]
        half, cols = ref.shape[0] // 2, ref.shape[1]
        own = ref.at[pl.ds(split * half, half), :]
        there = out.at[pl.ds(split * half, half), pl.ds(pl.multiple_of(owner * cols, cols), cols)]
        return own, there

    def w_copy(array, split, phase, mask):
        own, there = w_block(array, split, fs ^ mask)
        order = orders[split]
        slot = (array, split, (1 << phase) - 1 + sum(1 << i for i in range(phase) if mask & order[i]))
        return pltpu.make_async_remote_copy(
            src_ref=own if mask == 0 else there,
            dst_ref=there,
            send_sem=w_send.at[slot],
            recv_sem=w_recv.at[slot],
            device_id=(fs ^ order[phase], tp),
            device_id_type=MESH,
        )

    def r_block(array, owner):
        ref, out = rows[array]
        n = ref.shape[0]
        return out.at[pl.ds(pl.multiple_of(owner * n, n), n), :]

    def z_copy(array, way, step):
        sign = 1 if way == 0 else -1
        there = r_block(array, tp - sign * step * CORES)
        return pltpu.make_async_remote_copy(
            src_ref=rows[array][0] if step == 0 else there,
            dst_ref=there,
            send_sem=z_send.at[array, way, step],
            recv_sem=z_recv.at[array, way, step],
            device_id=(fs, tp + sign * CORES),
            device_id_type=MESH,
        )

    def sends(way, step):
        if way == 0:
            return jnp.logical_and(z - step >= 0, z < depth - 1)
        return jnp.logical_and(z + step <= depth - 1, z > 0)

    def arrives(way, step):
        return z - 1 - step >= 0 if way == 0 else z + 1 + step <= depth - 1

    def c_copy(array, way, step):
        sign = 1 if way == 0 else -1
        there = r_block(array, tp - sign * (step + 1) * CORES)
        slot = (array, way, step + 1)
        return pltpu.make_async_remote_copy(
            src_ref=rows[array][0] if step == -1 else there,
            dst_ref=there,
            send_sem=c_send.at[slot],
            recv_sem=c_recv.at[slot],
            device_id=(fs, tp ^ 1),
            device_id_type=MESH,
        )

    for array in range(2):
        for way in range(2):

            @pl.when(sends(way, 0))
            def _():
                z_copy(array, way, 0).start()

    for phase in range(phases):
        for array in range(3):
            for split in range(2):
                w_copy(array, split, phase, 0).start()
    for array in range(2):
        c_copy(array, 0, -1).start()
    local = []
    for array in range(3):
        for split in range(2):
            own, there = w_block(array, split, fs)
            local.append((own, there))
    for array in range(2):
        local.append((rows[array][0], r_block(array, tp)))
    local = [pltpu.make_async_copy(a, b, l_sem.at[i]) for i, (a, b) in enumerate(local)]
    for copy in local:
        copy.start()

    def w_event(array, phase, index):
        for split in range(2):
            order = orders[split]
            mask = sum(order[i] for i in range(phase) if index & (1 << i))
            w_copy(array, split, phase, mask).wait_recv()
            got = mask | order[phase]
            for later in range(phase + 1, phases):
                w_copy(array, split, later, got).start()

    def z_event(array, way, step):
        @pl.when(arrives(way, step))
        def _():
            z_copy(array, way, step).wait_recv()
            c_copy(array, way, step).start()

        if step + 1 < depth - 1:

            @pl.when(sends(way, step + 1))
            def _():
                z_copy(array, way, step + 1).start()

    w_events = [
        functools.partial(w_event, array, phase, index)
        for phase in range(phases)
        for index in range(1 << phase)
        for array in range(3)
    ]
    z_events = [
        [functools.partial(z_event, array, way, step) for way in range(2)]
        for step in range(depth - 1)
        for array in range(2)
    ]
    for i in range(max(len(w_events), len(z_events))):
        if i < len(w_events):
            w_events[i]()
        if i < len(z_events):
            for event in z_events[i]:
                event()

    for copy in local:
        copy.wait()
    for array in range(2):
        c_copy(array, 0, -1).wait_send()
        c_copy(array, 0, -1).wait_recv()
        for way in range(2):
            for step in range(depth - 1):

                @pl.when(sends(way, step))
                def _():
                    z_copy(array, way, step).wait_send()

                @pl.when(arrives(way, step))
                def _():
                    c_copy(array, way, step).wait_send()
                    c_copy(array, way, step).wait_recv()

    for array in range(3):
        for split in range(2):
            order = orders[split]
            for phase in range(phases):
                for index in range(1 << phase):
                    mask = sum(order[i] for i in range(phase) if index & (1 << i))
                    w_copy(array, split, phase, mask).wait_send()


def gather_all(n_fs, n_tp, *ins):
    tokens, gate, up, down, cot = ins
    depth = n_tp // CORES
    any_spec = pl.BlockSpec(memory_space=pl.ANY)
    vmem = pl.BlockSpec(memory_space=pltpu.VMEM)
    full = lambda a, axis, n: jax.ShapeDtypeStruct(
        tuple(s * n if i == axis else s for i, s in enumerate(a.shape)), a.dtype
    )
    dma = pltpu.SemaphoreType.DMA
    return pl.pallas_call(
        functools.partial(gather_kernel, n_fs, n_tp),
        out_shape=(
            full(tokens, 0, n_tp),
            full(gate, 1, n_fs),
            full(up, 1, n_fs),
            full(down, 1, n_fs),
            full(cot, 0, n_tp),
        ),
        in_specs=[vmem] * 5,
        out_specs=[any_spec] * 5,
        scratch_shapes=[
            dma((3, 2, n_fs - 1)),
            dma((3, 2, n_fs - 1)),
            dma((2, 2, max(depth - 1, 1))),
            dma((2, 2, max(depth - 1, 1))),
            dma((2, 2, depth)),
            dma((2, 2, depth)),
            dma((8,)),
        ],
        compiler_params=pltpu.CompilerParams(collective_id=0, has_side_effects=True),
        name="gather",
    )(*ins)


def scatter_kernel(n_fs, n_tp, *refs):
    gi_ref, *w_refs = refs[:4]
    gi_out, *w_outs = refs[4:8]
    stages, recvs = refs[8:11], refs[11:14]
    c_buf, z_stage, z_buf = refs[14:17]
    w_send, w_recv, z_send, z_recv, c_send, c_recv = refs[17:]
    fs, tp = lax.axis_index("fs"), lax.axis_index("tp")
    depth = n_tp // CORES
    z, core = tp // CORES, tp % CORES
    orders = orders_of(n_fs)
    phases = len(orders[0])
    f32 = jnp.float32
    greet(n_fs, depth, fs, tp, z)

    def w_own(array, split, mask):
        out = w_outs[array]
        half, cols = out.shape[0] // 2, out.shape[1]
        owner = fs ^ mask
        return w_refs[array].at[
            pl.ds(split * half, half), pl.ds(pl.multiple_of(owner * cols, cols), cols)
        ]

    def compact(order, mask):
        return sum(1 << i for i, bit in enumerate(order) if mask & bit)

    def w_copy(array, split, mask):
        order = orders[split]
        phase = first_bit(order, mask)
        slot = compact(order, mask) - 1
        src = w_own(array, split, mask) if phase == 0 else stages[array].at[split, slot]
        return pltpu.make_async_remote_copy(
            src_ref=src,
            dst_ref=recvs[array].at[split, slot],
            send_sem=w_send.at[array, split, slot],
            recv_sem=w_recv.at[array, split, slot],
            device_id=(fs ^ order[phase], tp),
            device_id_type=MESH,
        )

    def w_sum(array, split, mask):
        order = orders[split]
        total = w_own(array, split, mask)[...].astype(f32)
        limit = phases if mask == 0 else first_bit(order, mask)
        for phase in range(limit):
            sent = mask | order[phase]
            w_copy(array, split, sent).wait_recv()
            total += recvs[array][split, compact(order, sent) - 1].astype(f32)
        return total

    n = gi_out.shape[0]

    def g_rows(target, which):
        return pl.ds(pl.multiple_of((target * CORES + which) * n, n), n)

    def c_copy(target):
        return pltpu.make_async_remote_copy(
            src_ref=gi_ref.at[g_rows(target, 1 - core), :],
            dst_ref=c_buf.at[target],
            send_sem=c_send.at[target],
            recv_sem=c_recv.at[target],
            device_id=(fs, tp ^ 1),
            device_id_type=MESH,
        )

    def z_target(way, step):
        return depth - 1 - step if way == 0 else step

    def z_copy(way, step):
        return pltpu.make_async_remote_copy(
            src_ref=z_stage.at[way, step],
            dst_ref=z_buf.at[way, step],
            send_sem=z_send.at[way, step],
            recv_sem=z_recv.at[way, step],
            device_id=(fs, tp + CORES if way == 0 else tp - CORES),
            device_id_type=MESH,
        )

    def sends(way, step):
        t = z_target(way, step)
        return t > z if way == 0 else t < z

    def arrives(way, step):
        t = z_target(way, step)
        return jnp.logical_and(z > 0, t >= z) if way == 0 else jnp.logical_and(z < depth - 1, t <= z)

    targets = []
    for i in range(depth):
        t = depth - 1 - i // 2 if i % 2 == 0 else i // 2
        targets.append(t)
    for t in targets:
        c_copy(t).start()

    for array in range(3):
        for split in range(2):
            order = orders[split]
            masks = [m for m in range(1, n_fs) if m & order[0]]
            for mask in sorted(masks, key=lambda m: -compact(order, m)):
                w_copy(array, split, mask).start()

    both = c_buf
    for t in targets:
        c_copy(t).wait_recv()
        both[t] = (
            both[t].astype(f32) + gi_ref[g_rows(t, core), :].astype(f32)
        ).astype(both.dtype)

    def z_event(way, step):
        t = z_target(way, step)

        @pl.when(arrives(way, step))
        def _():
            z_copy(way, step).wait_recv()

        @pl.when(sends(way, step))
        def _():
            @pl.when(arrives(way, step))
            def _():
                z_stage[way, step] = (
                    both[t].astype(f32) + z_buf[way, step].astype(f32)
                ).astype(z_stage.dtype)

            @pl.when(jnp.logical_not(arrives(way, step)))
            def _():
                z_stage[way, step] = both[t]

            z_copy(way, step).start()

    def w_event(array, mask):
        for split in range(2):
            order = orders[split]
            real = sum(bit for i, bit in enumerate(order) if mask & (1 << i))
            slot = mask - 1
            stages[array][split, slot] = w_sum(array, split, real).astype(stages[array].dtype)
            w_copy(array, split, real).start()

    def w_finish(array):
        half = w_outs[array].shape[0] // 2
        for split in range(2):
            w_outs[array][pl.ds(split * half, half), :] = w_sum(array, split, 0)

    later = [m for m in range(1, n_fs) if not m & 1]
    later = sorted(later, key=lambda m: ((m & -m), -m))
    w_events = [functools.partial(w_event, array, mask) for array in range(3) for mask in later]
    z_events = [
        functools.partial(z_event, way, step) for step in range(depth - 1) for way in range(2)
    ]
    for event in z_events + w_events:
        event()

    total = both[z].astype(f32)
    zero = jnp.zeros_like(total)
    from_left = z_buf[0, jnp.clip(depth - 1 - z, 0, depth - 2)].astype(f32)
    from_right = z_buf[1, jnp.clip(z, 0, depth - 2)].astype(f32)
    total += jnp.where(z > 0, from_left, zero)
    total += jnp.where(z < depth - 1, from_right, zero)
    gi_out[...] = total.astype(gi_out.dtype)

    for array in range(3):
        w_finish(array)

    for t in targets:
        c_copy(t).wait_send()
    for way in range(2):
        for step in range(depth - 1):

            @pl.when(sends(way, step))
            def _():
                z_copy(way, step).wait_send()

    for array in range(3):
        for split in range(2):
            for mask in range(1, n_fs):
                w_copy(array, split, mask).wait_send()


def scatter_all(n_fs, n_tp, gi, gg, gu, gd):
    depth = n_tp // CORES
    f32 = jnp.float32
    vmem = pl.BlockSpec(memory_space=pltpu.VMEM)
    dma = pltpu.SemaphoreType.DMA
    shapes = tuple((g.shape[0], g.shape[1] // n_fs) for g in (gg, gu, gd))
    n, width = gi.shape[0] // n_tp, gi.shape[1]
    slots = [pltpu.VMEM((2, n_fs - 1, s[0] // 2, s[1]), gi.dtype) for s in shapes]
    return pl.pallas_call(
        functools.partial(scatter_kernel, n_fs, n_tp),
        out_shape=(jax.ShapeDtypeStruct((n, width), gi.dtype),)
        + tuple(jax.ShapeDtypeStruct(s, f32) for s in shapes),
        in_specs=[vmem] * 4,
        out_specs=[vmem] * 4,
        scratch_shapes=slots
        + slots
        + [
            pltpu.VMEM((depth, n, width), gi.dtype),
            pltpu.VMEM((2, depth - 1, n, width), gi.dtype),
            pltpu.VMEM((2, depth - 1, n, width), gi.dtype),
            dma((3, 2, n_fs - 1)),
            dma((3, 2, n_fs - 1)),
            dma((2, depth - 1)),
            dma((2, depth - 1)),
            dma((depth,)),
            dma((depth,)),
        ],
        compiler_params=pltpu.CompilerParams(
            collective_id=1, has_side_effects=True, vmem_limit_bytes=60 * 1024 * 1024
        ),
        name="scatter",
    )(gi, gg, gu, gd)


def body(n_fs, n_tp, tokens, gate_weight, up_weight, down_weight, grad_out):
    bf16 = tokens.dtype
    tok_all, gate_full, up_full, down_full, cot_all = gather_all(
        n_fs, n_tp, tokens, gate_weight.T, up_weight.T, down_weight, grad_out
    )
    gate_pre = over_cols(tok_all, gate_full)
    up_pre = over_cols(tok_all, up_full)
    sig_gate = jax.nn.sigmoid(gate_pre)
    active = gate_pre * sig_gate
    hidden = (active * up_pre).astype(bf16)
    d_hidden = over_cols(cot_all, down_full)
    d_gate = (d_hidden * up_pre * sig_gate * (1.0 + gate_pre * (1.0 - sig_gate))).astype(bf16)
    d_up = (d_hidden * active).astype(bf16)
    dot = functools.partial(jnp.dot, preferred_element_type=jnp.float32)
    grad_input = (dot(d_gate, gate_full) + dot(d_up, up_full)).astype(bf16)
    grad_input, grad_gate, grad_up, grad_down = scatter_all(
        n_fs,
        n_tp,
        grad_input,
        over_rows(d_gate, tok_all, bf16),
        over_rows(d_up, tok_all, bf16),
        over_rows(hidden, cot_all, bf16),
    )
    return grad_input, grad_gate.T, grad_up.T, grad_down


def solution(mesh):
    in_specs = (
        P(("fs", "tp"), None),
        P("fs", "tp"),
        P("fs", "tp"),
        P("tp", "fs"),
        P(("fs", "tp"), None),
    )
    out_specs = (P(("fs", "tp"), None), P("fs", "tp"), P("fs", "tp"), P("tp", "fs"))
    return jax.shard_map(
        functools.partial(body, mesh.shape["fs"], mesh.shape["tp"]),
        mesh=mesh,
        in_specs=in_specs,
        out_specs=out_specs,
        check_vma=False,
    )
```
